32 devices in a mesh: fs: 8 (over z, y), tp: 4 (over x, core).
Axes of the slice: x: 2, y: 2, z: 4, core: 2. Of those that a mesh axis runs over, the one named last changes fastest.
Arguments:
- prompt: bfloat16 [4096, 2048], P(('fs', 'tp')), may hold values from -6 to 6
- norm_gain: float32 [2048], P('fs'), may hold values from 0.1 to 1.9
- up_trained: float32 [2048, 8192], P('fs', 'tp'), may hold values from -0.125 to 0.125
- down_trained: float32 [2048, 8192], P('fs', 'tp'), may hold values from -0.0625 to 0.0625
Outputs:
- up_served: bfloat16 [2048, 8192], P(None, 'tp')
- down_served: bfloat16 [8192, 2048], P('tp')
- mixed: bfloat16 [4096, 2048], P(('fs', 'tp'))
The draws below stay inside these ranges and needn't reach their ends.
All inputs are finite; a program needn't handle non-finite values.
Results may differ from the reference program's by a relative error of at most 0.014.
Values may be sent and summed in bfloat16 or wider, within the bound.
A program may use at most 128 MiB of HBM per device.

```python
import jax
import jax.numpy as jnp
from jax import lax

D = 2048
FF = 8192
TOK_DEV = 128
TOKENS = 4096
N_FS = 8
N_TP = 4


def steps_of(rng, extent, split, least, high):
    def one(position, shards_of):
        steps = jax.random.uniform(jax.random.fold_in(jax.random.fold_in(rng, 6), position), (shards_of,), jnp.float32, least / len(split), high / len(split))
        return jnp.repeat(jnp.exp(steps), extent[position] // shards_of).reshape((-1,) + (1,) * (len(extent) - position - 1))

    loudness = one(*split[0])
    for cut in split[1:]:
        loudness = loudness * one(*cut)
    return loudness


def gaussian(stream_key, shape, deviation, reach, shards=(), kind=jnp.bfloat16):
    entries = jax.random.normal(stream_key, shape, jnp.float32) * deviation
    if len(shards) > 0:
        entries = steps_of(stream_key, shape, shards, -0.22, 0.18) * entries
    return jnp.clip(entries, min=-reach, max=reach).astype(kind)


def setup_inputs(seed: int = 0) -> dict:
    key_of = jax.random.split(jax.random.key(seed), 5)
    return {
        "prompt": gaussian(key_of[0], (TOKENS, D), 1.0, 6.0, ((0, 32),)),
        "norm_gain": jnp.clip(1.0 + 0.18 * jax.random.normal(key_of[1], (D,), jnp.float32), 0.1, 1.9),
        "up_trained": gaussian(key_of[2], (D, FF), D ** -0.5, 0.125, ((0, 8), (1, 4)), jnp.float32),
        "down_trained": gaussian(key_of[3], (D, FF), FF ** -0.5, 0.0625, ((0, 8), (1, 4)), jnp.float32),
    }


def reference(prompt, norm_gain, up_trained, down_trained):
    up_served = (norm_gain[:, None] * up_trained).astype(jnp.bfloat16)
    down_served = jnp.transpose(down_trained).astype(jnp.bfloat16)
    width = FF // N_TP
    groups = prompt.reshape(N_FS, N_TP * TOK_DEV, D)

    def one_group(rows):
        values = rows.astype(jnp.float32)
        scale = lax.rsqrt(lax.optimization_barrier(jnp.mean(values * values, axis=-1, keepdims=True)) + 1e-06)
        normed = (values * scale).astype(jnp.bfloat16)
        pre = jnp.dot(normed, up_served, preferred_element_type=jnp.float32)
        hidden = jnp.square(jax.nn.relu(pre)).astype(jnp.bfloat16)
        total = jnp.zeros((rows.shape[0], D), jnp.float32)
        for block in range(N_TP):
            partial_value = jnp.dot(hidden[:, block * width:(block + 1) * width], down_served[block * width:(block + 1) * width, :], preferred_element_type=jnp.float32).astype(jnp.bfloat16)
            total = total + partial_value.astype(jnp.float32)
        return total.astype(jnp.bfloat16)
    mixed = lax.map(one_group, groups).reshape(TOKENS, D)
    return (up_served, down_served, mixed)
```

```python
import functools

import jax
import jax.numpy as jnp
from jax import lax
from jax.experimental import pallas as pl
from jax.experimental.pallas import tpu as pltpu
from jax.sharding import PartitionSpec as P

MESH = pl.DeviceIdType.MESH
PIECES = 2


def factor(fs):
    ny = 1
    while ny * 2 * ny * 2 <= fs:
        ny *= 2
    return fs // ny, ny


def kernel(nz, ny, tp, prompt, gain, up_f, down_f, up_out, down_out, mixed,
           up_all, down_all, norm_all, hidden, part_send, part_recv,
           w_send, w_recv, n_send, n_recv, p_send, p_recv, l_sem):
    fs = nz * ny
    rows, width = up_f.shape
    piece = rows // PIECES
    tokens = prompt.shape[0]
    me = lax.axis_index("fs")
    t = lax.axis_index("tp")
    z, y = me // ny, lax.rem(me, ny)
    exists = (z < nz - 1, z > 0, y < ny - 1, y > 0)
    step = (ny, -ny, 1, -1)
    trick = ny == 2 and nz % 2 == 0
    half = PIECES // 2
    even = lax.rem(z, 2) == 0
    mate = z + 1 - 2 * lax.rem(z, 2)
    buffers = (up_all, down_all)
    sent = []

    barrier = pltpu.get_barrier_semaphore()
    for direction in range(4):
        @pl.when(exists[direction])
        def _():
            pl.semaphore_signal(barrier, inc=1, device_id={"fs": me + step[direction]}, device_id_type=MESH)
    for offset in range(1, tp):
        pl.semaphore_signal(barrier, inc=1, device_id={"tp": lax.rem(t + offset, tp)}, device_id_type=MESH)

    def weights(phase, block, c, direction):
        start = pl.multiple_of(block * rows + c * piece, piece)
        ref = buffers[phase].at[pl.ds(start, piece)]
        slot = (phase * fs + block) * PIECES + c
        return pltpu.make_async_remote_copy(
            src_ref=ref, dst_ref=ref,
            send_sem=w_send.at[direction, slot], recv_sem=w_recv.at[slot],
            device_id={"fs": me + step[direction]}, device_id_type=MESH)

    def send(condition, phase, block, c, direction):
        condition = jnp.logical_and(condition, exists[direction])
        sent.append((condition, phase, block, c, direction))

        @pl.when(condition)
        def _():
            weights(phase, block, c, direction).start()

    def arrive(condition, phase, block, c):
        @pl.when(condition)
        def _():
            weights(phase, block, c, 0).wait_recv()

    for c in range(PIECES):
        where = pl.ds(pl.multiple_of(me * rows + c * piece, piece), piece)
        part = slice(c * piece, (c + 1) * piece)
        up_all[where, :] = (gain[part, :] * up_f[part, :]).astype(jnp.bfloat16)
    pl.semaphore_wait(barrier, sum(e.astype(jnp.int32) for e in exists) + tp - 1)
    always = z >= 0
    for c in range(PIECES):
        for direction in range(4):
            send(always, 0, me, c, direction)

    values = prompt[...].astype(jnp.float32)
    scale = lax.rsqrt(jnp.mean(values * values, axis=-1, keepdims=True) + 1e-06)
    mine = pl.ds(pl.multiple_of(t * tokens, tokens), tokens)
    norm_all[mine, :] = (values * scale).astype(jnp.bfloat16)
    for c in range(PIECES):
        where = pl.ds(pl.multiple_of(me * rows + c * piece, piece), piece)
        part = slice(c * piece, (c + 1) * piece)
        down_all[where, :] = down_f[part, :].astype(jnp.bfloat16)

    def token_copy(offset):
        return pltpu.make_async_remote_copy(
            src_ref=norm_all.at[mine], dst_ref=norm_all.at[mine],
            send_sem=n_send.at[offset], recv_sem=n_recv.at[t],
            device_id={"tp": lax.rem(t + offset, tp)}, device_id_type=MESH)

    def token_arrival(offset):
        source = lax.rem(t + offset, tp)
        ref = norm_all.at[pl.ds(pl.multiple_of(source * tokens, tokens), tokens)]
        return pltpu.make_async_remote_copy(
            src_ref=ref, dst_ref=ref, send_sem=n_send.at[offset], recv_sem=n_recv.at[source],
            device_id={"tp": source}, device_id_type=MESH)

    for offset in range(1, tp):
        token_copy(offset).start()
    for c in range(half):
        for direction in (2, 3):
            send(always, 1, me, c, direction)

    def own_down(d):
        for c in range(PIECES):
            send(z == d, 1, me, c, 0)
            send(z == nz - 1 - d, 1, me, c, 1)

    def column(phase, d):
        for c in range(PIECES):
            for s in (1, -1):
                zb = z + s * d
                there = jnp.logical_and(zb >= 0, zb < nz)
                block = zb * ny + y
                arrive(there, phase, block, c)
                send(there, phase, block, c, 1 if s > 0 else 0)
                across = there
                if trick and c >= half:
                    across = jnp.logical_and(there, zb != mate)
                send(across, phase, block, c, 2)
                send(across, phase, block, c, 3)

    def swap(phase):
        if not trick:
            return
        block = z * ny + 1 - y
        for c in range(half, PIECES):
            if phase == 0:
                arrive(always, phase, block, c)
            send(even, phase, block, c, 0)
            send(jnp.logical_not(even), phase, block, c, 1)

    def sideways(phase, d, s):
        zb = z + s * d
        inside = jnp.logical_and(zb >= 0, zb < nz)
        for e in range(1, ny):
            for u in (1, -1):
                yb = y + u * e
                there = jnp.logical_and(inside, jnp.logical_and(yb >= 0, yb < ny))
                for c in range(PIECES):
                    if trick and phase == 0 and d == 0 and c >= half:
                        continue
                    wanted = there
                    if trick and c >= half:
                        wanted = jnp.logical_and(there, zb != mate)
                    arrive(wanted, phase, zb * ny + yb, c)
                    if e < ny - 1:
                        send(wanted, phase, zb * ny + yb, c, 3 if u > 0 else 2)

    def swapped(phase):
        if trick:
            for c in range(half, PIECES):
                arrive(always, phase, mate * ny + 1 - y, c)

    def partial_copy(block, offset):
        peer = lax.rem(t + offset, tp)
        return pltpu.make_async_remote_copy(
            src_ref=part_send.at[block, pl.ds(pl.multiple_of(peer * tokens, tokens), tokens)],
            dst_ref=part_recv.at[t, block],
            send_sem=p_send.at[offset], recv_sem=p_recv.at[t],
            device_id={"tp": peer}, device_id_type=MESH)

    def consume(condition, block):
        @pl.when(condition)
        def _():
            where = pl.ds(pl.multiple_of(block * rows, rows), rows)
            pltpu.make_async_copy(down_all.at[where], down_out.at[where], l_sem.at[1]).start()
            part_send[block] = lax.dot_general(
                hidden[...], down_all[where, :], (((1,), (1,)), ((), ())),
                preferred_element_type=jnp.float32).astype(jnp.bfloat16)
            for offset in range(1, tp):
                partial_copy(block, offset).start()

    def consume_column(d):
        @pl.loop(0, 1 if d == 0 else 2)
        def _(i):
            zb = z + (1 - 2 * i) * d
            consume(jnp.logical_and(zb >= 0, zb < nz), zb * ny + y)

    def consume_sideways(d):
        @pl.loop(0, (1 if d == 0 else 2) * (ny - 1))
        def _(i):
            zb = z + (1 - 2 * (i // (ny - 1))) * d
            yb = lax.rem(y + 1 + lax.rem(i, ny - 1), ny)
            inside = jnp.logical_and(zb >= 0, zb < nz)
            if trick:
                inside = jnp.logical_and(inside, zb != mate)
            consume(inside, zb * ny + yb)

    def signs(d):
        return (1,) if d == 0 else (1, -1)

    own_down(0)
    for d in range(1, nz):
        column(0, d)
        if d == 1:
            swap(0)
        own_down(d)
    for c in range(half, PIECES):
        for direction in (2, 3):
            send(always, 1, me, c, direction)
    for d in range(nz):
        for s in signs(d):
            sideways(0, d, s)
    swapped(0)
    up_copy = pltpu.make_async_copy(up_all, up_out, l_sem.at[0])
    up_copy.start()
    for offset in range(1, tp):
        token_arrival(offset).wait_recv()
    tile = 256

    @pl.loop(0, width // tile)
    def _(j):
        at = pl.ds(pl.multiple_of(j * tile, tile), tile)
        pre = jnp.dot(norm_all[...], up_all[:, at], preferred_element_type=jnp.float32)
        hidden[:, at] = jnp.square(jnp.maximum(pre, 0.0)).astype(jnp.bfloat16)

    for d in range(1, nz):
        column(1, d)
        if d == nz - 1:
            swap(1)
        consume_column(d - 1)
        if d == 1:
            sideways(1, 0, 1)
            consume_sideways(0)
    if nz == 1:
        sideways(1, 0, 1)
        consume_sideways(0)
    consume_column(nz - 1)
    for d in range(1, nz):
        for s in signs(d):
            sideways(1, d, s)
        consume_sideways(d)
    if trick:
        swapped(1)
        consume(always, mate * ny + 1 - y)

    for offset in range(1, tp):
        source = lax.rem(t + offset, tp)
        whole = part_recv.at[source]
        arrival = pltpu.make_async_remote_copy(
            src_ref=whole, dst_ref=whole, send_sem=p_send.at[offset], recv_sem=p_recv.at[source],
            device_id={"tp": source}, device_id_type=MESH)
        arrival.wait_recv()
    for block in range(fs):
        total = part_send[block, mine, :].astype(jnp.float32)
        for offset in range(1, tp):
            total += part_recv[lax.rem(t + offset, tp), block].astype(jnp.float32)
        mixed[:, block * rows:(block + 1) * rows] = total.astype(jnp.bfloat16)

    for offset in range(1, tp):
        token_copy(offset).wait_send()
        whole = part_recv.at[t]
        pltpu.make_async_remote_copy(
            src_ref=whole, dst_ref=whole, send_sem=p_send.at[offset], recv_sem=p_recv.at[t],
            device_id={"tp": lax.rem(t + offset, tp)}, device_id_type=MESH).wait_send()
    for condition, phase, block, c, direction in sent:
        @pl.when(condition)
        def _():
            weights(phase, block, c, direction).wait_send()
    up_copy.wait()
    pltpu.make_async_copy(down_all, down_out, l_sem.at[1]).wait()


def solution(mesh):
    fs, tp = mesh.shape["fs"], mesh.shape["tp"]
    nz, ny = factor(fs)

    def shards(prompt, norm_gain, up_trained, down_trained):
        rows, width = up_trained.shape
        tokens, depth = prompt.shape
        bf16 = jnp.bfloat16
        slots = 2 * fs * PIECES
        any_space = pl.BlockSpec(memory_space=pl.ANY)
        vmem = pl.BlockSpec(memory_space=pltpu.VMEM)
        up_whole, down_whole, mixed = pl.pallas_call(
            functools.partial(kernel, nz, ny, tp),
            out_shape=(
                jax.ShapeDtypeStruct((depth, width), bf16),
                jax.ShapeDtypeStruct((depth, width), bf16),
                jax.ShapeDtypeStruct((tokens, depth), bf16),
            ),
            in_specs=[vmem] * 4,
            out_specs=(any_space, any_space, vmem),
            scratch_shapes=[
                pltpu.VMEM((depth, width), bf16),
                pltpu.VMEM((depth, width), bf16),
                pltpu.VMEM((tp * tokens, depth), bf16),
                pltpu.VMEM((tp * tokens, width), bf16),
                pltpu.VMEM((fs, tp * tokens, rows), bf16),
                pltpu.VMEM((tp, fs, tokens, rows), bf16),
                pltpu.SemaphoreType.DMA((4, slots)),
                pltpu.SemaphoreType.DMA((slots,)),
                pltpu.SemaphoreType.DMA((tp,)),
                pltpu.SemaphoreType.DMA((tp,)),
                pltpu.SemaphoreType.DMA((tp,)),
                pltpu.SemaphoreType.DMA((tp,)),
                pltpu.SemaphoreType.DMA((2,)),
            ],
            compiler_params=pltpu.CompilerParams(
                collective_id=0, has_side_effects=True, vmem_limit_bytes=60 * 1024 * 1024
            ),
        )(prompt, norm_gain[:, None], up_trained, down_trained)
        return up_whole, jnp.transpose(down_whole), mixed

    return jax.shard_map(
        shards,
        mesh=mesh,
        in_specs=(P(("fs", "tp"), None), P("fs"), P("fs", "tp"), P("fs", "tp")),
        out_specs=(P(None, "tp"), P("tp", None), P(("fs", "tp"), None)),
        check_vma=False,
    )
```

```python
import functools

import jax
import jax.numpy as jnp
from jax import lax
from jax.experimental import pallas as pl
from jax.experimental.pallas import tpu as pltpu
from jax.sharding import PartitionSpec as P

MESH = pl.DeviceIdType.MESH
PIECES = 2
LIMIT = 40


def factor(fs):
    ny = 1
    while ny * 2 * ny * 2 <= fs:
        ny *= 2
    return fs // ny, ny


def turns(rows):
    return rows % 128 == 0


def flush(up_in, down_in, mixed_in, up_out, down_out, mixed_out, sems):
    copies = [
        pltpu.make_async_copy(source, target, sems.at[i])
        for i, (source, target) in enumerate(((up_in, up_out), (down_in, down_out), (mixed_in, mixed_out)))
    ]
    for copy in copies:
        copy.start()
    for copy in copies:
        copy.wait()


def kernel(nz, ny, tp, prompt, gain, up_f, down_f, up_all, down_out, mixed,
           down_scratch, norm_all, hidden, part_send, part_recv,
           w_send, w_recv, n_send, n_recv, p_send, p_recv):
    fs = nz * ny
    rows, width = up_f.shape
    tile = 256
    turned = turns(rows)
    down_all = down_scratch if turned else down_out
    piece = rows // PIECES
    tokens = prompt.shape[0]
    me = lax.axis_index("fs")
    t = lax.axis_index("tp")
    z, y = me // ny, lax.rem(me, ny)
    exists = (z < nz - 1, z > 0, y < ny - 1, y > 0)
    step = (ny, -ny, 1, -1)
    trick = ny == 2 and nz % 2 == 0
    half = PIECES // 2
    even = lax.rem(z, 2) == 0
    mate = z + 1 - 2 * lax.rem(z, 2)
    buffers = (up_all, down_all)
    sent = []

    barrier = pltpu.get_barrier_semaphore()
    for direction in range(4):
        @pl.when(exists[direction])
        def _():
            pl.semaphore_signal(barrier, inc=1, device_id={"fs": me + step[direction]}, device_id_type=MESH)
    for offset in range(1, tp):
        pl.semaphore_signal(barrier, inc=1, device_id={"tp": lax.rem(t + offset, tp)}, device_id_type=MESH)

    def weights(phase, block, c, direction):
        start = pl.multiple_of(block * rows + c * piece, piece)
        ref = buffers[phase].at[pl.ds(start, piece)]
        slot = (phase * fs + block) * PIECES + c
        return pltpu.make_async_remote_copy(
            src_ref=ref, dst_ref=ref,
            send_sem=w_send.at[direction, slot], recv_sem=w_recv.at[slot],
            device_id={"fs": me + step[direction]}, device_id_type=MESH)

    def send(condition, phase, block, c, direction):
        condition = jnp.logical_and(condition, exists[direction])
        sent.append((condition, phase, block, c, direction))

        @pl.when(condition)
        def _():
            weights(phase, block, c, direction).start()

    def arrive(condition, phase, block, c):
        @pl.when(condition)
        def _():
            weights(phase, block, c, 0).wait_recv()

    for c in range(PIECES):
        where = pl.ds(pl.multiple_of(me * rows + c * piece, piece), piece)
        part = slice(c * piece, (c + 1) * piece)
        up_all[where, :] = (gain[part, :] * up_f[part, :]).astype(jnp.bfloat16)
    pl.semaphore_wait(barrier, sum(e.astype(jnp.int32) for e in exists) + tp - 1)
    always = z >= 0
    for c in range(PIECES):
        for direction in range(4):
            send(always, 0, me, c, direction)

    values = prompt[...].astype(jnp.float32)
    scale = lax.rsqrt(jnp.mean(values * values, axis=-1, keepdims=True) + 1e-06)
    mine = pl.ds(pl.multiple_of(t * tokens, tokens), tokens)
    norm_all[mine, :] = (values * scale).astype(jnp.bfloat16)
    for c in range(PIECES):
        where = pl.ds(pl.multiple_of(me * rows + c * piece, piece), piece)
        part = slice(c * piece, (c + 1) * piece)
        down_all[where, :] = down_f[part, :].astype(jnp.bfloat16)

    def token_copy(offset):
        return pltpu.make_async_remote_copy(
            src_ref=norm_all.at[mine], dst_ref=norm_all.at[mine],
            send_sem=n_send.at[offset], recv_sem=n_recv.at[t],
            device_id={"tp": lax.rem(t + offset, tp)}, device_id_type=MESH)

    def token_arrival(offset):
        source = lax.rem(t + offset, tp)
        ref = norm_all.at[pl.ds(pl.multiple_of(source * tokens, tokens), tokens)]
        return pltpu.make_async_remote_copy(
            src_ref=ref, dst_ref=ref, send_sem=n_send.at[offset], recv_sem=n_recv.at[source],
            device_id={"tp": source}, device_id_type=MESH)

    for offset in range(1, tp):
        token_copy(offset).start()
    for c in range(half):
        for direction in (2, 3):
            send(always, 1, me, c, direction)

    def own_down(d):
        for c in range(PIECES):
            send(z == d, 1, me, c, 0)
            send(z == nz - 1 - d, 1, me, c, 1)

    def column(phase, d):
        for c in range(PIECES):
            for s in (1, -1):
                zb = z + s * d
                there = jnp.logical_and(zb >= 0, zb < nz)
                block = zb * ny + y
                arrive(there, phase, block, c)
                send(there, phase, block, c, 1 if s > 0 else 0)
                across = there
                if trick and c >= half:
                    across = jnp.logical_and(there, zb != mate)
                send(across, phase, block, c, 2)
                send(across, phase, block, c, 3)

    def swap(phase):
        if not trick:
            return
        block = z * ny + 1 - y
        for c in range(half, PIECES):
            if phase == 0:
                arrive(always, phase, block, c)
            send(even, phase, block, c, 0)
            send(jnp.logical_not(even), phase, block, c, 1)

    def sideways(phase, d, s):
        zb = z + s * d
        inside = jnp.logical_and(zb >= 0, zb < nz)
        for e in range(1, ny):
            for u in (1, -1):
                yb = y + u * e
                there = jnp.logical_and(inside, jnp.logical_and(yb >= 0, yb < ny))
                for c in range(PIECES):
                    if trick and phase == 0 and d == 0 and c >= half:
                        continue
                    wanted = there
                    if trick and c >= half:
                        wanted = jnp.logical_and(there, zb != mate)
                    arrive(wanted, phase, zb * ny + yb, c)
                    if e < ny - 1:
                        send(wanted, phase, zb * ny + yb, c, 3 if u > 0 else 2)

    def swapped(phase):
        if trick:
            for c in range(half, PIECES):
                arrive(always, phase, mate * ny + 1 - y, c)

    def partial_copy(block, offset):
        peer = lax.rem(t + offset, tp)
        return pltpu.make_async_remote_copy(
            src_ref=part_send.at[block, pl.ds(pl.multiple_of(peer * tokens, tokens), tokens)],
            dst_ref=part_recv.at[t, block],
            send_sem=p_send.at[offset], recv_sem=p_recv.at[t],
            device_id={"tp": peer}, device_id_type=MESH)

    def consume(condition, block):
        @pl.when(condition)
        def _():
            where = pl.ds(pl.multiple_of(block * rows, rows), rows)
            part_send[block] = lax.dot_general(
                hidden[...], down_all[where, :], (((1,), (1,)), ((), ())),
                preferred_element_type=jnp.float32).astype(jnp.bfloat16)
            for offset in range(1, tp):
                partial_copy(block, offset).start()
            if turned:
                @pl.loop(0, width // tile)
                def _(j):
                    at = pl.ds(pl.multiple_of(j * tile, tile), tile)
                    down_out[at, where] = jnp.transpose(down_all[where, at])

    def consume_column(d):
        @pl.loop(0, 1 if d == 0 else 2)
        def _(i):
            zb = z + (1 - 2 * i) * d
            consume(jnp.logical_and(zb >= 0, zb < nz), zb * ny + y)

    def consume_sideways(d):
        @pl.loop(0, (1 if d == 0 else 2) * (ny - 1))
        def _(i):
            zb = z + (1 - 2 * (i // (ny - 1))) * d
            yb = lax.rem(y + 1 + lax.rem(i, ny - 1), ny)
            inside = jnp.logical_and(zb >= 0, zb < nz)
            if trick:
                inside = jnp.logical_and(inside, zb != mate)
            consume(inside, zb * ny + yb)

    def signs(d):
        return (1,) if d == 0 else (1, -1)

    own_down(0)
    for d in range(1, nz):
        column(0, d)
        if d == 1:
            swap(0)
        own_down(d)
    for c in range(half, PIECES):
        for direction in (2, 3):
            send(always, 1, me, c, direction)
    for d in range(nz):
        for s in signs(d):
            sideways(0, d, s)
    swapped(0)
    for offset in range(1, tp):
        token_arrival(offset).wait_recv()

    @pl.loop(0, width // tile)
    def _(j):
        at = pl.ds(pl.multiple_of(j * tile, tile), tile)
        pre = jnp.dot(norm_all[...], up_all[:, at], preferred_element_type=jnp.float32)
        hidden[:, at] = jnp.square(jnp.maximum(pre, 0.0)).astype(jnp.bfloat16)

    for d in range(1, nz):
        column(1, d)
        if d == nz - 1:
            swap(1)
        consume_column(d - 1)
        if d == 1:
            sideways(1, 0, 1)
            consume_sideways(0)
    if nz == 1:
        sideways(1, 0, 1)
        consume_sideways(0)
    consume_column(nz - 1)
    for d in range(1, nz):
        for s in signs(d):
            sideways(1, d, s)
        consume_sideways(d)
    if trick:
        swapped(1)
        consume(always, mate * ny + 1 - y)

    for offset in range(1, tp):
        source = lax.rem(t + offset, tp)
        whole = part_recv.at[source]
        arrival = pltpu.make_async_remote_copy(
            src_ref=whole, dst_ref=whole, send_sem=p_send.at[offset], recv_sem=p_recv.at[source],
            device_id={"tp": source}, device_id_type=MESH)
        arrival.wait_recv()
    for block in range(fs):
        total = part_send[block, mine, :].astype(jnp.float32)
        for offset in range(1, tp):
            total += part_recv[lax.rem(t + offset, tp), block].astype(jnp.float32)
        mixed[:, block * rows:(block + 1) * rows] = total.astype(jnp.bfloat16)

    for offset in range(1, tp):
        token_copy(offset).wait_send()
        whole = part_recv.at[t]
        pltpu.make_async_remote_copy(
            src_ref=whole, dst_ref=whole, send_sem=p_send.at[offset], recv_sem=p_recv.at[t],
            device_id={"tp": lax.rem(t + offset, tp)}, device_id_type=MESH).wait_send()
    for condition, phase, block, c, direction in sent:
        @pl.when(condition)
        def _():
            weights(phase, block, c, direction).wait_send()


def solution(mesh):
    fs, tp = mesh.shape["fs"], mesh.shape["tp"]
    nz, ny = factor(fs)

    def shards(prompt, norm_gain, up_trained, down_trained):
        rows, width = up_trained.shape
        tokens, depth = prompt.shape
        bf16 = jnp.bfloat16
        turned = turns(rows)
        down_shape = (width, depth) if turned else (depth, width)
        slots = 2 * fs * PIECES
        any_space = pl.BlockSpec(memory_space=pl.ANY)
        vmem = pl.BlockSpec(memory_space=pltpu.VMEM)
        up_whole, down_whole, mixed = pl.pallas_call(
            functools.partial(kernel, nz, ny, tp),
            out_shape=(
                pltpu.VMEM((depth, width), bf16),
                pltpu.VMEM(down_shape, bf16),
                pltpu.VMEM((tokens, depth), bf16),
            ),
            in_specs=[vmem] * 4,
            out_specs=[vmem] * 3,
            scratch_shapes=[
                pltpu.VMEM((depth, width) if turned else (16, 128), bf16),
                pltpu.VMEM((tp * tokens, depth), bf16),
                pltpu.VMEM((tp * tokens, width), bf16),
                pltpu.VMEM((fs, tp * tokens, rows), bf16),
                pltpu.VMEM((tp, fs, tokens, rows), bf16),
                pltpu.SemaphoreType.DMA((4, slots)),
                pltpu.SemaphoreType.DMA((slots,)),
                pltpu.SemaphoreType.DMA((tp,)),
                pltpu.SemaphoreType.DMA((tp,)),
                pltpu.SemaphoreType.DMA((tp,)),
                pltpu.SemaphoreType.DMA((tp,)),
            ],
            compiler_params=pltpu.CompilerParams(
                collective_id=0, has_side_effects=True, vmem_limit_bytes=LIMIT * 1024 * 1024
            ),
        )(prompt, norm_gain[:, None], up_trained, down_trained)
        up_whole, down_whole, mixed = pl.pallas_call(
            flush,
            out_shape=(
                jax.ShapeDtypeStruct((depth, width), bf16),
                jax.ShapeDtypeStruct(down_shape, bf16),
                jax.ShapeDtypeStruct((tokens, depth), bf16),
            ),
            in_specs=[vmem] * 3,
            out_specs=[any_space] * 3,
            scratch_shapes=[pltpu.SemaphoreType.DMA((3,))],
            compiler_params=pltpu.CompilerParams(vmem_limit_bytes=2 * 1024 * 1024),
        )(up_whole, down_whole, mixed)
        return up_whole, down_whole if turned else jnp.transpose(down_whole), mixed

    return jax.shard_map(
        shards,
        mesh=mesh,
        in_specs=(P(("fs", "tp"), None), P("fs"), P("fs", "tp"), P("fs", "tp")),
        out_specs=(P(None, "tp"), P("tp", None), P(("fs", "tp"), None)),
        check_vma=False,
    )
```

```python
import functools

import jax
import jax.numpy as jnp
from jax import lax
from jax.experimental import pallas as pl
from jax.experimental.pallas import tpu as pltpu
from jax.sharding import PartitionSpec as P

MESH = pl.DeviceIdType.MESH
LIMIT = 40


def factor(fs):
    ny = 1
    while ny * 2 * ny * 2 <= fs:
        ny *= 2
    return fs // ny, ny


def pieces_of(rows):
    return max(2, rows // 64)


def turns(rows):
    return rows % 128 == 0


def flush(up_in, down_in, mixed_in, up_out, down_out, mixed_out, sems):
    copies = [
        pltpu.make_async_copy(source, target, sems.at[i])
        for i, (source, target) in enumerate(((up_in, up_out), (down_in, down_out), (mixed_in, mixed_out)))
    ]
    for copy in copies:
        copy.start()
    for copy in copies:
        copy.wait()


def kernel(nz, ny, tp, prompt, gain, up_f, down_f, up_all, down_out, mixed,
           down_scratch, norm_all, hidden, part_send, part_recv,
           w_send, w_recv, n_send, n_recv, p_send, p_recv):
    fs = nz * ny
    rows, width = up_f.shape
    pieces = pieces_of(rows)
    tile = 256
    turned = turns(rows)
    down_all = down_scratch if turned else down_out
    piece = rows // pieces
    tokens = prompt.shape[0]
    me = lax.axis_index("fs")
    t = lax.axis_index("tp")
    z, y = me // ny, lax.rem(me, ny)
    exists = (z < nz - 1, z > 0, y < ny - 1, y > 0)
    step = (ny, -ny, 1, -1)
    trick = ny == 2 and nz % 2 == 0
    half = pieces // 2
    even = lax.rem(z, 2) == 0
    mate = z + 1 - 2 * lax.rem(z, 2)
    buffers = (up_all, down_all)
    sent = []

    barrier = pltpu.get_barrier_semaphore()
    for direction in range(4):
        @pl.when(exists[direction])
        def _():
            pl.semaphore_signal(barrier, inc=1, device_id={"fs": me + step[direction]}, device_id_type=MESH)
    for offset in range(1, tp):
        pl.semaphore_signal(barrier, inc=1, device_id={"tp": lax.rem(t + offset, tp)}, device_id_type=MESH)

    def weights(phase, block, c, direction):
        start = pl.multiple_of(block * rows + c * piece, piece)
        ref = buffers[phase].at[pl.ds(start, piece)]
        slot = (phase * fs + block) * pieces + c
        return pltpu.make_async_remote_copy(
            src_ref=ref, dst_ref=ref,
            send_sem=w_send.at[direction, slot], recv_sem=w_recv.at[slot],
            device_id={"fs": me + step[direction]}, device_id_type=MESH)

    def send(condition, phase, block, c, direction):
        condition = jnp.logical_and(condition, exists[direction])
        sent.append((condition, phase, block, c, direction))

        @pl.when(condition)
        def _():
            weights(phase, block, c, direction).start()

    def arrive(condition, phase, block, c):
        @pl.when(condition)
        def _():
            weights(phase, block, c, 0).wait_recv()

    for c in range(pieces):
        where = pl.ds(pl.multiple_of(me * rows + c * piece, piece), piece)
        part = slice(c * piece, (c + 1) * piece)
        up_all[where, :] = (gain[part, :] * up_f[part, :]).astype(jnp.bfloat16)
    pl.semaphore_wait(barrier, sum(e.astype(jnp.int32) for e in exists) + tp - 1)
    always = z >= 0
    for c in range(pieces):
        for direction in range(4):
            send(always, 0, me, c, direction)

    values = prompt[...].astype(jnp.float32)
    scale = lax.rsqrt(jnp.mean(values * values, axis=-1, keepdims=True) + 1e-06)
    mine = pl.ds(pl.multiple_of(t * tokens, tokens), tokens)
    norm_all[mine, :] = (values * scale).astype(jnp.bfloat16)
    for c in range(pieces):
        where = pl.ds(pl.multiple_of(me * rows + c * piece, piece), piece)
        part = slice(c * piece, (c + 1) * piece)
        down_all[where, :] = down_f[part, :].astype(jnp.bfloat16)

    def token_copy(offset):
        return pltpu.make_async_remote_copy(
            src_ref=norm_all.at[mine], dst_ref=norm_all.at[mine],
            send_sem=n_send.at[offset], recv_sem=n_recv.at[t],
            device_id={"tp": lax.rem(t + offset, tp)}, device_id_type=MESH)

    def token_arrival(offset):
        source = lax.rem(t + offset, tp)
        ref = norm_all.at[pl.ds(pl.multiple_of(source * tokens, tokens), tokens)]
        return pltpu.make_async_remote_copy(
            src_ref=ref, dst_ref=ref, send_sem=n_send.at[offset], recv_sem=n_recv.at[source],
            device_id={"tp": source}, device_id_type=MESH)

    for offset in range(1, tp):
        token_copy(offset).start()
    for c in range(half):
        for direction in (2, 3):
            send(always, 1, me, c, direction)

    def own_down(d):
        for c in range(pieces):
            send(z == d, 1, me, c, 0)
            send(z == nz - 1 - d, 1, me, c, 1)

    def column(phase, d):
        for c in range(pieces):
            for s in (1, -1):
                zb = z + s * d
                there = jnp.logical_and(zb >= 0, zb < nz)
                block = zb * ny + y
                arrive(there, phase, block, c)
                send(there, phase, block, c, 1 if s > 0 else 0)
                across = there
                if trick and c >= half:
                    across = jnp.logical_and(there, zb != mate)
                send(across, phase, block, c, 2)
                send(across, phase, block, c, 3)

    def swap(phase):
        if not trick:
            return
        block = z * ny + 1 - y
        for c in range(half, pieces):
            if phase == 0:
                arrive(always, phase, block, c)
            send(even, phase, block, c, 0)
            send(jnp.logical_not(even), phase, block, c, 1)

    def sideways(phase, d, s):
        zb = z + s * d
        inside = jnp.logical_and(zb >= 0, zb < nz)
        for e in range(1, ny):
            for u in (1, -1):
                yb = y + u * e
                there = jnp.logical_and(inside, jnp.logical_and(yb >= 0, yb < ny))
                for c in range(pieces):
                    if trick and phase == 0 and d == 0 and c >= half:
                        continue
                    wanted = there
                    if trick and c >= half:
                        wanted = jnp.logical_and(there, zb != mate)
                    arrive(wanted, phase, zb * ny + yb, c)
                    if e < ny - 1:
                        send(wanted, phase, zb * ny + yb, c, 3 if u > 0 else 2)

    def swapped(phase):
        if trick:
            for c in range(half, pieces):
                arrive(always, phase, mate * ny + 1 - y, c)

    def partial_copy(block, offset):
        peer = lax.rem(t + offset, tp)
        return pltpu.make_async_remote_copy(
            src_ref=part_send.at[block, pl.ds(pl.multiple_of(peer * tokens, tokens), tokens)],
            dst_ref=part_recv.at[t, block],
            send_sem=p_send.at[offset], recv_sem=p_recv.at[t],
            device_id={"tp": peer}, device_id_type=MESH)

    def consume(condition, block):
        @pl.when(condition)
        def _():
            where = pl.ds(pl.multiple_of(block * rows, rows), rows)
            part_send[block] = lax.dot_general(
                hidden[...], down_all[where, :], (((1,), (1,)), ((), ())),
                preferred_element_type=jnp.float32).astype(jnp.bfloat16)
            for offset in range(1, tp):
                partial_copy(block, offset).start()
            if turned:
                @pl.loop(0, width // tile)
                def _(j):
                    at = pl.ds(pl.multiple_of(j * tile, tile), tile)
                    down_out[at, where] = jnp.transpose(down_all[where, at])

    def consume_column(d):
        @pl.loop(0, 1 if d == 0 else 2)
        def _(i):
            zb = z + (1 - 2 * i) * d
            consume(jnp.logical_and(zb >= 0, zb < nz), zb * ny + y)

    def consume_sideways(d):
        @pl.loop(0, (1 if d == 0 else 2) * (ny - 1))
        def _(i):
            zb = z + (1 - 2 * (i // (ny - 1))) * d
            yb = lax.rem(y + 1 + lax.rem(i, ny - 1), ny)
            inside = jnp.logical_and(zb >= 0, zb < nz)
            if trick:
                inside = jnp.logical_and(inside, zb != mate)
            consume(inside, zb * ny + yb)

    def signs(d):
        return (1,) if d == 0 else (1, -1)

    own_down(0)
    for d in range(1, nz):
        column(0, d)
        if d == 1:
            swap(0)
        own_down(d)
    for c in range(half, pieces):
        for direction in (2, 3):
            send(always, 1, me, c, direction)
    for d in range(nz):
        for s in signs(d):
            sideways(0, d, s)
    swapped(0)
    for offset in range(1, tp):
        token_arrival(offset).wait_recv()

    @pl.loop(0, width // tile)
    def _(j):
        at = pl.ds(pl.multiple_of(j * tile, tile), tile)
        pre = jnp.dot(norm_all[...], up_all[:, at], preferred_element_type=jnp.float32)
        hidden[:, at] = jnp.square(jnp.maximum(pre, 0.0)).astype(jnp.bfloat16)

    for d in range(1, nz):
        column(1, d)
        if d == nz - 1:
            swap(1)
        consume_column(d - 1)
        if d == 1:
            sideways(1, 0, 1)
            consume_sideways(0)
    if nz == 1:
        sideways(1, 0, 1)
        consume_sideways(0)
    consume_column(nz - 1)
    for d in range(1, nz):
        for s in signs(d):
            sideways(1, d, s)
        consume_sideways(d)
    if trick:
        swapped(1)
        consume(always, mate * ny + 1 - y)

    for offset in range(1, tp):
        source = lax.rem(t + offset, tp)
        whole = part_recv.at[source]
        arrival = pltpu.make_async_remote_copy(
            src_ref=whole, dst_ref=whole, send_sem=p_send.at[offset], recv_sem=p_recv.at[source],
            device_id={"tp": source}, device_id_type=MESH)
        arrival.wait_recv()
    for block in range(fs):
        total = part_send[block, mine, :].astype(jnp.float32)
        for offset in range(1, tp):
            total += part_recv[lax.rem(t + offset, tp), block].astype(jnp.float32)
        mixed[:, block * rows:(block + 1) * rows] = total.astype(jnp.bfloat16)

    for offset in range(1, tp):
        token_copy(offset).wait_send()
        whole = part_recv.at[t]
        pltpu.make_async_remote_copy(
            src_ref=whole, dst_ref=whole, send_sem=p_send.at[offset], recv_sem=p_recv.at[t],
            device_id={"tp": lax.rem(t + offset, tp)}, device_id_type=MESH).wait_send()
    for condition, phase, block, c, direction in sent:
        @pl.when(condition)
        def _():
            weights(phase, block, c, direction).wait_send()


def solution(mesh):
    fs, tp = mesh.shape["fs"], mesh.shape["tp"]
    nz, ny = factor(fs)

    def shards(prompt, norm_gain, up_trained, down_trained):
        rows, width = up_trained.shape
        tokens, depth = prompt.shape
        bf16 = jnp.bfloat16
        turned = turns(rows)
        down_shape = (width, depth) if turned else (depth, width)
        slots = 2 * fs * pieces_of(rows)
        any_space = pl.BlockSpec(memory_space=pl.ANY)
        vmem = pl.BlockSpec(memory_space=pltpu.VMEM)
        up_whole, down_whole, mixed = pl.pallas_call(
            functools.partial(kernel, nz, ny, tp),
            out_shape=(
                pltpu.VMEM((depth, width), bf16),
                pltpu.VMEM(down_shape, bf16),
                pltpu.VMEM((tokens, depth), bf16),
            ),
            in_specs=[vmem] * 4,
            out_specs=[vmem] * 3,
            scratch_shapes=[
                pltpu.VMEM((depth, width) if turned else (16, 128), bf16),
                pltpu.VMEM((tp * tokens, depth), bf16),
                pltpu.VMEM((tp * tokens, width), bf16),
                pltpu.VMEM((fs, tp * tokens, rows), bf16),
                pltpu.VMEM((tp, fs, tokens, rows), bf16),
                pltpu.SemaphoreType.DMA((4, slots)),
                pltpu.SemaphoreType.DMA((slots,)),
                pltpu.SemaphoreType.DMA((tp,)),
                pltpu.SemaphoreType.DMA((tp,)),
                pltpu.SemaphoreType.DMA((tp,)),
                pltpu.SemaphoreType.DMA((tp,)),
            ],
            compiler_params=pltpu.CompilerParams(
                collective_id=0, has_side_effects=True, vmem_limit_bytes=LIMIT * 1024 * 1024
            ),
        )(prompt, norm_gain[:, None], up_trained, down_trained)
        up_whole, down_whole, mixed = pl.pallas_call(
            flush,
            out_shape=(
                jax.ShapeDtypeStruct((depth, width), bf16),
                jax.ShapeDtypeStruct(down_shape, bf16),
                jax.ShapeDtypeStruct((tokens, depth), bf16),
            ),
            in_specs=[vmem] * 3,
            out_specs=[any_space] * 3,
            scratch_shapes=[pltpu.SemaphoreType.DMA((3,))],
            compiler_params=pltpu.CompilerParams(vmem_limit_bytes=2 * 1024 * 1024),
        )(up_whole, down_whole, mixed)
        return up_whole, down_whole if turned else jnp.transpose(down_whole), mixed

    return jax.shard_map(
        shards,
        mesh=mesh,
        in_specs=(P(("fs", "tp"), None), P("fs"), P("fs", "tp"), P("fs", "tp")),
        out_specs=(P(None, "tp"), P("tp", None), P(("fs", "tp"), None)),
        check_vma=False,
    )
```
